32 devices in a mesh: ep: 16 (over z, y, x), tp: 2 (over core).
Axes of the slice: x: 2, y: 2, z: 4, core: 2. Of those that a mesh axis runs over, the one named last changes fastest.
Arguments:
- tokens: bfloat16 [384, 2048], P('ep'), may hold values from -6 to 6
- attn_gain: float32 [2048], replicated, may hold values from 0.1 to 1.9
- w_query: bfloat16 [2048, 1024], P(None, 'tp'), may hold values from -0.125 to 0.125
- w_key: bfloat16 [2048, 1024], P(None, 'tp'), may hold values from -0.125 to 0.125
- w_value: bfloat16 [2048, 1024], P(None, 'tp'), may hold values from -0.125 to 0.125
- w_zgate: bfloat16 [2048, 1024], P(None, 'tp'), may hold values from -0.125 to 0.125
- w_decay: bfloat16 [2048, 8], P(None, 'tp'), may hold values from -0.125 to 0.125
- w_beta: bfloat16 [2048, 8], P(None, 'tp'), may hold values from -0.125 to 0.125
- decay_rate: float32 [8], P('tp'), may hold values from 0.05 to 2
- decay_bias: float32 [8], P('tp'), may hold values from -3 to 3
- state: float32 [384, 8, 128, 128], P('ep', 'tp'), may hold values from -2 to 2
- out_gain: float32 [128], replicated, may hold values from 0.1 to 1.9
- w_out: bfloat16 [1024, 2048], P('tp'), may hold values from -0.1875 to 0.1875
- ffn_gain: float32 [2048], replicated, may hold values from 0.1 to 1.9
- expert_gate: bfloat16 [16, 2048, 512], P('ep', None, 'tp'), may hold values from -0.125 to 0.125
- expert_up: bfloat16 [16, 2048, 512], P('ep', None, 'tp'), may hold values from -0.125 to 0.125
- expert_down: bfloat16 [16, 512, 2048], P('ep', 'tp'), may hold values from -0.25 to 0.25
- routes: int32 [384, 2], P('ep'), may hold values from 0 to 15, all different within a row; in each aligned block of 24 rows (0 to 23, 24 to 47, ...) at most 6 rows name the same one
- route_weight: float32 [384, 2], P('ep'), may hold values from 0.2 to 1
Outputs:
- layer_out: bfloat16 [384, 2048], P('ep', 'tp')
- new_state: float32 [384, 8, 128, 128], P('ep', 'tp')
The draws below stay inside these ranges and needn't reach their ends.
Inputs may be any that keep to these rules, and one draw needn't show every extreme that they name: `routes`: the 2 entries of a row differ. Among the rows of one index of ep (aligned blocks of 24 rows) no expert is named more than 6 times, a bound that some block reaches.
All inputs are finite; a program needn't handle non-finite values.
Results may differ from the reference program's by a relative error of at most 0.014.
Values may be sent and summed in bfloat16 or wider, within the bound.
No kernel may reach another device: no remote copies, remote signals or barrier semaphores. Data moves between devices by JAX's collectives and lax.ppermute only.
A program may use at most 128 MiB of HBM per device.

```python
import math
import jax
import jax.numpy as jnp
import numpy as np
from jax import lax

D = 2048
HEADS = 8
HEAD_DIM = 128
FF_EXP = 512
TOP_K = 2
SEQS_DEV = 24
SEQS = 384
EXPERTS = 16
CAP = 6
N_EP = 16
N_TP = 2


def levels(stream_key, shape, cuts, least, top_value):
    def one(position, blocks):
        draws = jax.random.uniform(jax.random.fold_in(jax.random.fold_in(stream_key, 6), position), (blocks,), jnp.float32, least / len(cuts), top_value / len(cuts))
        return jnp.repeat(jnp.exp(draws), shape[position] // blocks).reshape((-1,) + (1,) * (len(shape) - position - 1))

    factor_of = one(*cuts[0])
    for cut in cuts[1:]:
        factor_of = factor_of * one(*cut)
    return factor_of


def deal_out(rng, own, number, rows, count, top, reach, lean):
    sequence = jax.random.permutation(rng, count)
    heavy_load, ordinary = shares(count, rows * top, reach, lean, True), shares(count, rows * top, reach, lean, False)
    places = jnp.arange(count)

    def named(tallies, rotation):
        used = int((tallies > 0).sum())
        fixed = max(1, used // 4)
        moved = fixed + (places - fixed + rotation * (used - fixed)) % max(1, count - fixed)
        return jnp.zeros((count,), jnp.int32).at[sequence[jnp.where(places < fixed, places, moved)]].set(jnp.asarray(tallies, jnp.int32))

    tallies = jnp.where(number % 4 == 0, named(heavy_load, number // 4), named(ordinary, number - number // 4 - 1))
    mixed = jax.random.permutation(jax.random.fold_in(own, 3), count)
    giver, sink = mixed[0:count // 2 * 2:2], mixed[1:count // 2 * 2:2]
    slack = jnp.minimum(tallies[giver] - 1, reach - tallies[sink]) // 2
    slack = jnp.where((giver == sequence[0]) | (sink == sequence[0]) | (tallies[sink] == 0), 0, jnp.maximum(slack, 0))
    moved = jax.random.randint(jax.random.fold_in(own, 4), (count // 2,), 0, 1 << 20) % (slack + 1)
    tallies = tallies.at[giver].add(-moved).at[sink].add(moved)
    items = jnp.searchsorted(jnp.cumsum(tallies), jnp.arange(rows * top), side="right").astype(jnp.int32)
    listing = items.reshape(top, rows).T
    listing = listing[jax.random.permutation(jax.random.fold_in(own, 1), rows)]
    rotation = jax.random.randint(jax.random.fold_in(own, 2), (rows, 1), 0, top)
    return jnp.take_along_axis(listing, (jnp.arange(top)[None, :] + rotation) % top, axis=1)


def shares(amount, total, reach, slope, full):
    weights = [(1 << 20) // math.isqrt(rank ** slope) + 1 for rank in range(1, amount + 1)]
    largest = reach if full else min(reach, max(-(-total // amount), total * weights[0] // sum(weights)))
    least = 1 if total - largest >= amount - 1 else 0
    counts, rest = [largest] + [least] * (amount - 1), total - largest - least * (amount - 1)
    while rest > 0:
        movable = [i for i in range(1, amount) if counts[i] < largest] or [i for i in range(1, amount) if counts[i] < reach]
        pool, budget = sum([weights[i] for i in movable]), rest
        for i in movable:
            extra = min(reach - counts[i], max(1, budget * weights[i] // pool), rest)
            counts[i] = counts[i] + extra
            rest = rest - extra
    return np.array(counts)


def normal_values(stream_key, dims, width, limit, shards=(), kind=jnp.bfloat16):
    entries = width * jax.random.normal(stream_key, dims, jnp.float32)
    if shards:
        entries = entries * levels(stream_key, dims, shards, -0.22, 0.18)
    return jnp.clip(entries, -limit, limit).astype(kind)


def setup_inputs(seed: int = 0) -> dict:
    streams_of = jax.random.split(jax.random.key(seed), 20)
    tokens = normal_values(streams_of[0], (SEQS, D), 1.0, 6.0, ((0, 16),))
    attn_gain = jnp.clip(1.0 + 0.18 * jax.random.normal(streams_of[1], (D,), jnp.float32), 0.1, 1.9)
    w_query = normal_values(streams_of[2], (D, HEADS * HEAD_DIM), D ** -0.5, 0.125, ((1, 2),))
    w_key = normal_values(streams_of[3], (D, HEADS * HEAD_DIM), D ** -0.5, 0.125, ((1, 2),))
    w_value = normal_values(streams_of[4], (D, HEADS * HEAD_DIM), D ** -0.5, 0.125, ((1, 2),))
    w_zgate = normal_values(streams_of[5], (D, HEADS * HEAD_DIM), D ** -0.5, 0.125, ((1, 2),))
    w_decay = normal_values(streams_of[6], (D, HEADS), D ** -0.5, 0.125, ((1, 2),))
    w_beta = normal_values(streams_of[7], (D, HEADS), D ** -0.5, 0.125, ((1, 2),))
    decay_rate = jnp.clip(jnp.exp(math.log(2.0) - 3.6888794 * jax.random.uniform(streams_of[8], (HEADS,), jnp.float32) ** levels(streams_of[8], (HEADS,), ((0, 2),), -0.2, 0.2)), 0.05, 2.0)
    decay_bias = normal_values(streams_of[9], (HEADS,), 1.0, 3.0, ((0, 2),), jnp.float32)
    state = normal_values(streams_of[10], (SEQS, HEADS, HEAD_DIM, HEAD_DIM), 0.3, 2.0, ((0, 16), (1, 2)), jnp.float32)
    out_gain = jnp.clip(1.0 + 0.18 * jax.random.normal(streams_of[11], (HEAD_DIM,), jnp.float32), 0.1, 1.9)
    w_out = normal_values(streams_of[12], (HEADS * HEAD_DIM, D), (HEADS * HEAD_DIM) ** -0.5, 0.1875, ((0, 2),))
    ffn_gain = jnp.clip(1.0 + 0.18 * jax.random.normal(streams_of[13], (D,), jnp.float32), 0.1, 1.9)
    expert_gate = normal_values(streams_of[14], (EXPERTS, D, FF_EXP), D ** -0.5, 0.125, ((0, 16), (2, 2)))
    expert_up = normal_values(streams_of[15], (EXPERTS, D, FF_EXP), D ** -0.5, 0.125, ((0, 16), (2, 2)))
    expert_down = normal_values(streams_of[16], (EXPERTS, FF_EXP, D), FF_EXP ** -0.5, 0.25, ((0, 16), (1, 2)))
    routes_keys = jax.random.split(jax.random.fold_in(streams_of[17], 1), SEQS // SEQS_DEV)
    routes_turns = jax.random.permutation(jax.random.fold_in(streams_of[17], 3), SEQS // SEQS_DEV)
    routes = jax.vmap(lambda own, number: deal_out(jax.random.fold_in(streams_of[17], 2), own, number, SEQS_DEV, EXPERTS, TOP_K, CAP, 2))(routes_keys, routes_turns).reshape((SEQS, TOP_K))
    route_weight = jnp.clip(0.2 + 0.8 * jax.random.uniform(streams_of[18], (SEQS, TOP_K), jnp.float32) ** levels(streams_of[18], (SEQS, TOP_K), ((0, 16),), -0.2, 0.2), 0.2, 1.0)
    return dict(tokens=tokens, attn_gain=attn_gain, w_query=w_query, w_key=w_key, w_value=w_value, w_zgate=w_zgate, w_decay=w_decay, w_beta=w_beta, decay_rate=decay_rate, decay_bias=decay_bias, state=state, out_gain=out_gain, w_out=w_out, ffn_gain=ffn_gain, expert_gate=expert_gate, expert_up=expert_up, expert_down=expert_down, routes=routes, route_weight=route_weight)


EPS = 1e-06

def rms_scale(rows, gain):
    return rows * lax.rsqrt(lax.optimization_barrier(jnp.mean(rows * rows, axis=-1, keepdims=True)) + EPS) * gain

def unit_rows(rows):
    return rows * lax.rsqrt(lax.optimization_barrier(jnp.sum(rows * rows, axis=-1, keepdims=True)) + EPS)

def mixer_block(args):
    normed, w_query, w_key, w_value, w_zgate, w_decay, w_beta, decay_rate, decay_bias, state, out_gain = args
    seqs = normed.shape[0]

    def project(weight):
        return jnp.dot(normed, weight, preferred_element_type=jnp.float32).astype(jnp.bfloat16)

    def heads_of(raw):
        return raw.reshape(seqs, HEADS, HEAD_DIM).astype(jnp.float32)
    query = unit_rows(jax.nn.silu(heads_of(project(w_query)))) * HEAD_DIM ** (-0.5)
    key = unit_rows(jax.nn.silu(heads_of(project(w_key))))
    value = jax.nn.silu(heads_of(project(w_value)))
    zmul = jax.nn.silu(heads_of(project(w_zgate)))
    fade = jnp.exp(-decay_rate * jax.nn.softplus(project(w_decay).astype(jnp.float32) + decay_bias))
    beta = jax.nn.sigmoid(project(w_beta).astype(jnp.float32))
    predicted = jnp.einsum('shkv,shk->shv', state, key, precision=lax.Precision.HIGHEST)
    written = beta[..., None] * (value - fade[..., None] * predicted)
    updated = fade[..., None, None] * state + key[..., :, None] * written[..., None, :]
    read = jnp.einsum('shkv,shk->shv', updated, query, precision=lax.Precision.HIGHEST)
    heads_out = (rms_scale(read, out_gain) * zmul).astype(jnp.bfloat16)
    return (heads_out.reshape(seqs, HEADS * HEAD_DIM), updated)

def reference(tokens, attn_gain, w_query, w_key, w_value, w_zgate, w_decay, w_beta, decay_rate, decay_bias, state, out_gain, w_out, ffn_gain, expert_gate, expert_up, expert_down, routes, route_weight):
    resid_in = tokens.astype(jnp.float32)
    normed = rms_scale(resid_in, attn_gain).astype(jnp.bfloat16)

    def one_block(args):
        block_rows, block_state = args
        return mixer_block((block_rows, w_query, w_key, w_value, w_zgate, w_decay, w_beta, decay_rate, decay_bias, block_state, out_gain))
    heads_out, new_state = lax.map(one_block, (normed.reshape(N_EP, SEQS_DEV, D), state.reshape(N_EP, SEQS_DEV, HEADS, HEAD_DIM, HEAD_DIM)))
    heads_out = heads_out.reshape(SEQS, HEADS * HEAD_DIM)
    new_state = new_state.reshape(SEQS, HEADS, HEAD_DIM, HEAD_DIM)
    group = HEADS * HEAD_DIM // N_TP
    mixed = jnp.zeros((SEQS, D), jnp.float32)
    for part in range(N_TP):
        term = jnp.dot(heads_out[:, part * group:(part + 1) * group], w_out[part * group:(part + 1) * group], preferred_element_type=jnp.float32)
        mixed = mixed + term.astype(jnp.bfloat16).astype(jnp.float32)
    resid = resid_in + mixed
    moe_in = rms_scale(resid, ffn_gain).astype(jnp.bfloat16)
    flat = routes.reshape(N_EP, SEQS_DEV * TOP_K)
    onehot = (flat[..., None] == jnp.arange(EXPERTS, dtype=jnp.int32)[None, None, :]).astype(jnp.int32)
    before = jnp.cumsum(onehot, axis=1) - onehot
    slot = lax.optimization_barrier(jnp.sum(before * onehot, axis=-1)).astype(jnp.int32)
    block_ids = jnp.broadcast_to(jnp.arange(N_EP, dtype=jnp.int32)[:, None], flat.shape)
    row_of = (jnp.arange(SEQS_DEV * TOP_K, dtype=jnp.int32) // TOP_K)[None, :] + SEQS_DEV * block_ids
    table = jnp.zeros((EXPERTS, N_EP, CAP), jnp.int32).at[flat, block_ids, slot].set(row_of.astype(jnp.int32))
    piece = FF_EXP // N_TP

    def run_expert(args):
        w_gate, w_up, w_down, picks = args
        rows = moe_in[picks.reshape(-1)]
        gate = jnp.dot(rows, w_gate, preferred_element_type=jnp.float32)
        up = jnp.dot(rows, w_up, preferred_element_type=jnp.float32)
        hidden = (jax.nn.silu(gate) * up).astype(jnp.bfloat16)
        total = jnp.zeros((rows.shape[0], D), jnp.float32)
        for part in range(N_TP):
            term = jnp.dot(hidden[:, part * piece:(part + 1) * piece], w_down[part * piece:(part + 1) * piece], preferred_element_type=jnp.float32)
            total = total + term.astype(jnp.bfloat16).astype(jnp.float32)
        return total.astype(jnp.bfloat16).reshape(N_EP, CAP, D)
    results = lax.map(run_expert, (expert_gate, expert_up, expert_down, table))
    per_route = results[flat, block_ids, slot].astype(jnp.float32).reshape(SEQS, TOP_K, D)
    combined = lax.optimization_barrier(jnp.sum(per_route * route_weight[..., None], axis=1))
    layer_out = (resid + combined).astype(jnp.bfloat16)
    return (layer_out, new_state)
```

```python
import jax
import jax.numpy as jnp
from jax import lax
from jax.experimental import pallas as pl
from jax.experimental.pallas import tpu as pltpu
from jax.sharding import PartitionSpec as P

EPS = 1e-06
BF16 = jnp.bfloat16
F32 = jnp.float32


def rms_scale(rows, gain):
    return rows * lax.rsqrt(jnp.mean(rows * rows, axis=-1, keepdims=True) + EPS) * gain


def unit_rows(rows):
    return rows * lax.rsqrt(jnp.sum(rows * rows, axis=-1, keepdims=True) + EPS)


def silu(x):
    return x * jax.nn.sigmoid(x)


def chunk_of(seqs):
    return next(c for c in (4, 3, 2, 1) if seqs % c == 0)


def mixer_kernel(
    tokens_ref, again_ref, wa_ref, wb_ref, rate_ref, bias_ref, ogain_ref,
    wq_hbm, wk_hbm, wv_hbm, wz_hbm, state_hbm, wo_hbm,
    part_ref, new_hbm,
    wq, wk, wv, wz, wo, st, kq, vb, fb, bb, rd, zb, wsem, isem, osem,
):
    seqs, heads, dim, _ = st.shape
    chunk = chunk_of(seqs)
    chunks = seqs // chunk

    def weight(i):
        src, dst = ((wk_hbm, wk), (wq_hbm, wq), (wv_hbm, wv), (wz_hbm, wz), (wo_hbm, wo))[i]
        return pltpu.make_async_copy(src, dst, wsem.at[i])

    def rows_of(c):
        return pl.ds(c * chunk, chunk)

    def state_in(c):
        return pltpu.make_async_copy(state_hbm.at[rows_of(c)], st.at[rows_of(c)], isem.at[c])

    def state_out(c):
        return pltpu.make_async_copy(st.at[rows_of(c)], new_hbm.at[rows_of(c)], osem.at[c])

    for i in range(3):
        weight(i).start()
    for c in range(chunks):
        state_in(c).start()
    weight(3).start()
    weight(4).start()

    normed = rms_scale(tokens_ref[...].astype(F32), again_ref[...]).astype(BF16)

    def narrow(ref):
        raw = lax.dot_general(normed, ref[...], (((1,), (1,)), ((), ())), preferred_element_type=F32)
        return raw.astype(BF16).astype(F32)

    raw_a = narrow(wa_ref) + bias_ref[...]
    softplus = jnp.maximum(raw_a, 0.0) + jnp.log1p(jnp.exp(-jnp.abs(raw_a)))
    fade = jnp.exp(-rate_ref[...] * softplus)
    beta = jax.nn.sigmoid(narrow(wb_ref))
    for h in range(heads):
        fb[:, h, :] = jnp.broadcast_to(fade[:, h : h + 1], (seqs, dim))
        bb[:, h, :] = jnp.broadcast_to(beta[:, h : h + 1], (seqs, dim))

    def project(ref):
        raw = jnp.dot(normed, ref[...], preferred_element_type=F32)
        return silu(raw.astype(BF16).astype(F32))

    def head(x, h):
        return x[:, h * dim : (h + 1) * dim]

    weight(0).wait()
    key = project(wk)
    for h in range(heads):
        kq[:, h, :] = unit_rows(head(key, h))
    weight(1).wait()
    query = project(wq)
    for h in range(heads):
        kq[:, heads + h, :] = unit_rows(head(query, h)) * dim ** (-0.5)
    weight(2).wait()
    value = project(wv)
    for h in range(heads):
        vb[:, h, :] = head(value, h)

    def body(c, carry):
        state_in(c).wait()
        for i in range(chunk):
            s = c * chunk + i
            turned = kq[s].T
            fades, betas, values = fb[s], bb[s], vb[s]
            for h in range(heads):
                old = st[s, h] * fades[h : h + 1]
                kcol = turned[:, h : h + 1]
                qcol = turned[:, heads + h : heads + h + 1]
                predicted = jnp.sum(old * kcol, axis=0, keepdims=True)
                written = betas[h : h + 1] * (values[h : h + 1] - predicted)
                new = old + kcol * written
                st[s, h] = new
                rd[s, pl.ds(h, 1), :] = jnp.sum(new * qcol, axis=0, keepdims=True)
        state_out(c).start()
        return carry

    lax.fori_loop(0, chunks, body, 0)
    weight(3).wait()
    zb[...] = project(wz)
    outs = []
    for h in range(heads):
        outs.append((rms_scale(rd[:, h, :], ogain_ref[...]) * head(zb[...], h)).astype(BF16))
    weight(4).wait()
    part_ref[...] = jnp.dot(
        jnp.concatenate(outs, axis=1), wo[...], preferred_element_type=F32
    ).astype(BF16)
    for c in range(chunks):
        state_out(c).wait()


def mixer(tokens, attn_gain, wq, wk, wv, wz, wa, wb, rate, bias, state, out_gain, wo):
    seqs, width = tokens.shape
    heads, dim = state.shape[1:3]
    chunks = seqs // chunk_of(seqs)
    vm = pl.BlockSpec(memory_space=pltpu.VMEM)
    hbm = pl.BlockSpec(memory_space=pl.ANY)
    flat = heads * dim
    return pl.pallas_call(
        mixer_kernel,
        out_shape=(
            jax.ShapeDtypeStruct((seqs, wo.shape[1]), BF16),
            jax.ShapeDtypeStruct(state.shape, F32),
        ),
        in_specs=[vm] * 7 + [hbm] * 6,
        out_specs=(vm, hbm),
        scratch_shapes=[pltpu.VMEM((width, flat), BF16)] * 4
        + [pltpu.VMEM(wo.shape, BF16), pltpu.VMEM(state.shape, F32)]
        + [pltpu.VMEM((seqs, 2 * heads, dim), F32)]
        + [pltpu.VMEM((seqs, heads, dim), F32)] * 4
        + [pltpu.VMEM((seqs, flat), F32)]
        + [
            pltpu.SemaphoreType.DMA((5,)),
            pltpu.SemaphoreType.DMA((chunks,)),
            pltpu.SemaphoreType.DMA((chunks,)),
        ],
        compiler_params=pltpu.CompilerParams(vmem_limit_bytes=48 << 20),
        name="mixer",
    )(
        tokens, attn_gain[None], wa.T, wb.T, rate[None], bias[None], out_gain[None],
        wq, wk, wv, wz, state, wo,
    )


def dispatch_kernel(side_ref, tokens_ref, part_ref, other_ref, gain_ref, pick_ref, out_ref, res_ref, buf):
    mixed = part_ref[...].astype(F32) + other_ref[...].astype(F32)
    buf[...] = tokens_ref[...].astype(F32) + mixed
    resid = buf[...]
    cols = out_ref.shape[1]
    own = pl.ds(pl.multiple_of(side_ref[0] * cols, cols), cols)
    scale = lax.rsqrt(jnp.mean(resid * resid, axis=-1, keepdims=True) + EPS)
    own_resid = buf[:, own]
    moe_in = (own_resid * scale * gain_ref[:, own]).astype(BF16)
    out_ref[...] = jnp.dot(pick_ref[...], moe_in, preferred_element_type=F32).astype(BF16)
    res_ref[...] = own_resid


def dispatch(side, tokens, part, other, gain, pick, cols):
    seqs, width = tokens.shape
    vm = pl.BlockSpec(memory_space=pltpu.VMEM)
    return pl.pallas_call(
        dispatch_kernel,
        out_shape=(
            jax.ShapeDtypeStruct((pick.shape[0], cols), BF16),
            jax.ShapeDtypeStruct((seqs, cols), F32),
        ),
        in_specs=[pl.BlockSpec(memory_space=pltpu.SMEM)] + [vm] * 5,
        out_specs=(vm, vm),
        scratch_shapes=[pltpu.VMEM((seqs, width), F32)],
        name="dispatch",
    )(side, tokens, part, other, gain[None], pick)


def expert_kernel(side_ref, own_ref, oth_ref, wg_hbm, wu_hbm, wd_hbm, mine_ref, send_ref, wg, wu, wd, sem):
    copies = [
        pltpu.make_async_copy(src.at[0], dst, sem.at[i])
        for i, (src, dst) in enumerate(((wg_hbm, wg), (wu_hbm, wu), (wd_hbm, wd)))
    ]
    for copy in copies:
        copy.start()
    cols = own_ref.shape[1]
    side = side_ref[0]
    own = pl.ds(pl.multiple_of(side * cols, cols), cols)
    oth = pl.ds(pl.multiple_of((1 - side) * cols, cols), cols)

    def project(ref):
        return jnp.dot(own_ref[...], ref[own, :], preferred_element_type=F32) + jnp.dot(
            oth_ref[...], ref[oth, :], preferred_element_type=F32
        )

    copies[0].wait()
    gate = silu(project(wg))
    copies[1].wait()
    hidden = (gate * project(wu)).astype(BF16)
    copies[2].wait()
    send_ref[...] = jnp.dot(hidden, wd[:, oth], preferred_element_type=F32).astype(BF16)
    mine_ref[...] = jnp.dot(hidden, wd[:, own], preferred_element_type=F32).astype(BF16)


def expert(side, own, oth, wg, wu, wd):
    vm = pl.BlockSpec(memory_space=pltpu.VMEM)
    hbm = pl.BlockSpec(memory_space=pl.ANY)
    half = jax.ShapeDtypeStruct(own.shape, BF16)
    return pl.pallas_call(
        expert_kernel,
        out_shape=(half, half),
        in_specs=[pl.BlockSpec(memory_space=pltpu.SMEM), vm, vm, hbm, hbm, hbm],
        out_specs=(vm, vm),
        scratch_shapes=[pltpu.VMEM(w.shape[1:], BF16) for w in (wg, wu, wd)]
        + [pltpu.SemaphoreType.DMA((3,))],
        name="expert",
    )(side, own, oth, wg, wu, wd)


def per_device(
    tokens,
    attn_gain,
    w_query,
    w_key,
    w_value,
    w_zgate,
    w_decay,
    w_beta,
    decay_rate,
    decay_bias,
    state,
    out_gain,
    w_out,
    ffn_gain,
    expert_gate,
    expert_up,
    expert_down,
    routes,
    route_weight,
):
    seqs, width = tokens.shape
    top = routes.shape[1]
    swap = [(0, 1), (1, 0)]
    experts = lax.axis_size("ep")
    cap = max(2, 2 * seqs * top // experts)
    columns = width // lax.axis_size("tp")
    side = lax.axis_index("tp").astype(jnp.int32).reshape(1)
    partial_value, new_state = mixer(
        tokens, attn_gain, w_query, w_key, w_value, w_zgate, w_decay, w_beta,
        decay_rate, decay_bias, state, out_gain, w_out,
    )
    other = lax.ppermute(partial_value, "tp", swap)

    flat_routes = routes.reshape(-1)
    onehot = (flat_routes[:, None] == jnp.arange(experts, dtype=jnp.int32)[None, :]).astype(jnp.int32)
    before = jnp.cumsum(onehot, axis=0) - onehot
    slot = jnp.sum(before * onehot, axis=1)
    place = flat_routes * cap + slot
    slots = jnp.arange(experts * cap, dtype=jnp.int32)
    pick = (place[:, None] == slots[None, :]).astype(BF16)
    taken = jnp.any(place.reshape(1, seqs, top) == slots[:, None, None], axis=2).astype(BF16)

    outgoing, own_resid = dispatch(side, tokens, partial_value, other, ffn_gain, taken, columns)
    outgoing = outgoing.reshape(experts, cap, columns)
    arrived = lax.all_to_all(outgoing, "ep", split_axis=0, concat_axis=0, tiled=True)
    rows = arrived.reshape(experts * cap, columns)
    mine, send = expert(side, rows, lax.ppermute(rows, "tp", swap), expert_gate, expert_up, expert_down)
    summed = (mine.astype(F32) + lax.ppermute(send, "tp", swap).astype(F32)).astype(BF16)
    summed = summed.reshape(experts, cap, columns)
    returned = lax.all_to_all(summed, "ep", split_axis=0, concat_axis=0, tiled=True)
    returned = returned.reshape(experts * cap, columns)
    per_route = jnp.dot(pick, returned, preferred_element_type=F32).reshape(seqs, top, columns)
    combined = jnp.sum(per_route * route_weight[..., None], axis=1)
    layer_out = (own_resid + combined).astype(BF16)
    return (layer_out, new_state)


def solution(mesh):
    in_specs = (
        P("ep", None),
        P(),
        P(None, "tp"),
        P(None, "tp"),
        P(None, "tp"),
        P(None, "tp"),
        P(None, "tp"),
        P(None, "tp"),
        P("tp"),
        P("tp"),
        P("ep", "tp", None, None),
        P(),
        P("tp", None),
        P(),
        P("ep", None, "tp"),
        P("ep", None, "tp"),
        P("ep", "tp", None),
        P("ep", None),
        P("ep", None),
    )
    out_specs = (P("ep", "tp"), P("ep", "tp", None, None))
    return jax.shard_map(
        per_device, mesh=mesh, in_specs=in_specs, out_specs=out_specs, check_vma=False
    )
```
